32 devices in a mesh: sp: 8 (over z, core), tp: 4 (over y, x).
Axes of the slice: x: 2, y: 2, z: 4, core: 2. Of those that a mesh axis runs over, the one named last changes fastest.
Arguments:
- layer_input: bfloat16 [8192, 4096], P('sp', 'tp'), may hold values from -6 to 6
- key_weight: bfloat16 [4096, 4096], P(None, 'tp'), may hold values from -0.09375 to 0.09375
- value_weight: bfloat16 [4096, 4096], P(None, 'tp'), may hold values from -0.09375 to 0.09375
- decay_exponent: float32 [32], P('tp'), may hold values from -0.077 to -0.00016845703, as said below
- query_new: bfloat16 [2, 4096], P(None, 'tp'), may hold values from -6 to 6
- key_new: bfloat16 [2, 4096], P(None, 'tp'), may hold values from -6 to 6
- value_new: bfloat16 [2, 4096], P(None, 'tp'), may hold values from -6 to 6
- norm_gain: float32 [4096], P('tp'), may hold values from 0.1 to 1.9
Outputs:
- state_cache: bfloat16 [2, 32, 128, 128], P(None, 'tp', 'sp')
- first_read: bfloat16 [2, 4096], P(None, 'tp')
The draws below stay inside these ranges and needn't reach their ends.
Inputs may be any that keep to these rules, and one draw needn't show every extreme that they name: decay_exponent is negative.
All inputs are finite; a program needn't handle non-finite values.
Results may differ from the reference program's by a relative error of at most 0.011.
Values may be sent and summed in bfloat16 or wider, within the bound.
No kernel may reach another device: no remote copies, remote signals or barrier semaphores. Data moves between devices by JAX's collectives and lax.ppermute only.
A program may use at most 64 MiB of HBM per device.

```python
import jax
import jax.numpy as jnp
from jax import lax

D = 4096
HEADS = 32
DK = 128
DV = 128
SEQS = 2
TOKENS = 8192
LEN = 4096


def draw_decay_exponent(key, part):
    first_key = jax.random.fold_in(key, 11)
    second_key = jax.random.fold_in(key, 12)
    third_key = jax.random.fold_in(key, 13)
    slow_share = 0.5
    slow_flag = jax.random.uniform(first_key, (HEADS,), jnp.float32) < slow_share
    fast_rate = jax.random.uniform(second_key, (HEADS,), jnp.float32, 2.3026 / 100.0, 2.3026 / 30.0)
    slow_rate = jax.random.uniform(third_key, (HEADS,), jnp.float32, 0.3, 1.0) * (2.3026 / LEN)
    return -jnp.where(slow_flag, slow_rate, fast_rate)


def levels(rng, dims, shards, least, largest):
    def one(dim, parts):
        draws = jax.random.uniform(jax.random.fold_in(jax.random.fold_in(rng, 6), dim), (parts,), jnp.float32, least / len(shards), largest / len(shards))
        return jnp.repeat(jnp.exp(draws), dims[dim] // parts).reshape((-1,) + (1,) * (len(dims) - dim - 1))

    gain = one(*shards[0])
    for cut in shards[1:]:
        gain = gain * one(*cut)
    return gain


def bell_draw(stream_key, extent, spread, most, split=(), kind=jnp.bfloat16):
    result = spread * jax.random.normal(stream_key, extent, jnp.float32)
    if split:
        result = result * levels(stream_key, extent, split, -0.22, 0.18)
    return jnp.clip(result, -most, most).astype(kind)


def setup_inputs(seed: int = 0) -> dict:
    key_of = jax.random.split(jax.random.key(seed), 9)
    return {
        "layer_input": bell_draw(key_of[0], (TOKENS, D), 1.0, 6.0, ((0, 8), (1, 4))),
        "key_weight": bell_draw(key_of[1], (D, HEADS * DK), D ** -0.5, 0.09375, ((1, 4),)),
        "value_weight": bell_draw(key_of[2], (D, HEADS * DV), D ** -0.5, 0.09375, ((1, 4),)),
        "decay_exponent": draw_decay_exponent(jax.random.fold_in(key_of[8], 71), 0),
        "query_new": bell_draw(key_of[4], (SEQS, HEADS * DK), 1.0, 6.0, ((1, 4),)),
        "key_new": bell_draw(key_of[5], (SEQS, HEADS * DK), 1.0, 6.0, ((1, 4),)),
        "value_new": bell_draw(key_of[6], (SEQS, HEADS * DV), 1.0, 6.0, ((1, 4),)),
        "norm_gain": jnp.clip(1.0 + 0.18 * jax.random.normal(key_of[7], (HEADS * DV,), jnp.float32), 0.1, 1.9),
    }


def rotate(projected, position):
    half_width = projected.shape[-1] // 2
    inverse = 1.0 / 10000.0 ** jnp.linspace(0.0, 1.0, half_width, dtype=jnp.float32)
    angle = position[:, None] * inverse[None, :]
    cosine = jnp.cos(angle)[:, None, :]
    sine = jnp.sin(angle)[:, None, :]
    first = projected[..., :half_width]
    second = projected[..., half_width:]
    return jnp.concatenate([first * cosine - second * sine, first * sine + second * cosine], axis=-1)

def reference(layer_input, key_weight, value_weight, decay_exponent, query_new, key_new, value_new, norm_gain):
    key_proj = jnp.dot(layer_input, key_weight, preferred_element_type=jnp.float32)
    value_proj = jnp.dot(layer_input, value_weight, preferred_element_type=jnp.float32)
    position = (jnp.arange(TOKENS, dtype=jnp.int32) % LEN).astype(jnp.float32)
    keys = (rotate(key_proj.reshape(TOKENS, HEADS, DK), position) * DK ** (-0.5)).astype(jnp.bfloat16)
    values = value_proj.astype(jnp.bfloat16).reshape(TOKENS, HEADS, DV)
    distance = LEN - 1.0 - position
    weighting = jnp.exp(decay_exponent[None, :] * distance[:, None])
    weighted = (keys.astype(jnp.float32) * weighting[:, :, None]).astype(jnp.bfloat16)
    final = jnp.einsum('slhd,slhe->shde', weighted.astype(jnp.float32).reshape(SEQS, LEN, HEADS, DK), values.astype(jnp.float32).reshape(SEQS, LEN, HEADS, DV), precision=lax.Precision.HIGHEST)
    state_cache = final.astype(jnp.bfloat16)
    queries = query_new.astype(jnp.float32).reshape(SEQS, HEADS, DK)
    keys_next = key_new.astype(jnp.float32).reshape(SEQS, HEADS, DK)
    values_next = value_new.astype(jnp.float32).reshape(SEQS, HEADS, DV)
    carried = jnp.einsum('shd,shde->she', queries, final, precision=lax.Precision.HIGHEST)
    own_term = lax.optimization_barrier(jnp.sum(queries * keys_next, axis=2))[:, :, None] * values_next
    mixed = jnp.exp(decay_exponent)[None, :, None] * carried + own_term
    normed = mixed * lax.rsqrt(lax.optimization_barrier(jnp.mean(mixed * mixed, axis=2, keepdims=True)) + 1e-06)
    normed = normed * norm_gain.reshape(HEADS, DV)[None, :, :]
    return (state_cache, normed.reshape(SEQS, HEADS * DV).astype(jnp.bfloat16))
```

```python
import jax
import jax.numpy as jnp
from jax import lax
from jax.sharding import PartitionSpec as P

SEQS = 2
LATE = 2


def turn_tables(position, half_width, scale):
    inverse = 1.0 / 10000.0 ** jnp.linspace(0.0, 1.0, half_width, dtype=jnp.float32)
    angle = position[:, None] * inverse[None, :]
    return jnp.cos(angle) * scale, jnp.sin(angle) * scale


def swap(block, axis, mask):
    size = lax.axis_size(axis)
    return lax.ppermute(block, axis, [(i, i ^ mask) for i in range(size)])


def spread(own, axis):
    size = lax.axis_size(axis)
    bits = [1 << b for b in range(size.bit_length() - 1)]
    rows = own.shape[0] // 2
    halves = []
    for half, order in enumerate((bits, bits[::-1])):
        pieces = {0: [own[half * rows : (half + 1) * rows]]}
        for bit in order:
            for mask in list(pieces):
                blocks = pieces[mask]
                if mask and bit == order[-1]:
                    blocks = [cut for block in blocks for cut in jnp.split(block, LATE)]
                pieces[mask | bit] = [swap(block, axis, bit) for block in blocks]
        halves.append(pieces)
    return halves


def on_device(
    layer_input, key_weight, value_weight, decay_exponent, query_new, key_new, value_new, norm_gain
):
    tok_count, feature_local = layer_input.shape
    head_local = decay_exponent.shape[0]
    key_width = key_weight.shape[1] // head_local
    value_width = value_weight.shape[1] // head_local
    half_width = key_width // 2
    sp_size = lax.axis_size("sp")
    seq_span = sp_size // SEQS
    seq_length = tok_count * seq_span
    sp_place = lax.axis_index("sp")
    tp_place = lax.axis_index("tp")

    position = (sp_place % seq_span * tok_count + jnp.arange(tok_count, dtype=jnp.int32)).astype(
        jnp.float32
    )
    cosine, sine = turn_tables(position, half_width, key_width ** (-0.5))
    distance = seq_length - 1.0 - position
    weighting = jnp.exp(decay_exponent[None, :] * distance[:, None])

    def term(piece, mask, weight):
        rows = lax.dynamic_slice_in_dim(weight, (tp_place ^ mask) * feature_local, feature_local)
        return jnp.dot(piece, rows, preferred_element_type=jnp.float32)

    def total(terms):
        result = terms[0]
        for other in terms[1:]:
            result = result + other
        return result

    state = None
    start = 0
    for pieces in spread(layer_input, "tp"):
        early = {mask: blocks[0] for mask, blocks in pieces.items() if len(blocks) == 1}
        late = {mask: blocks for mask, blocks in pieces.items() if len(blocks) > 1}
        key_early = total([term(piece, mask, key_weight) for mask, piece in early.items()])
        value_early = total([term(piece, mask, value_weight) for mask, piece in early.items()])
        size = key_early.shape[0] // LATE
        for step in range(LATE):
            cut = slice(step * size, (step + 1) * size)
            key_late = [term(blocks[step], mask, key_weight) for mask, blocks in late.items()]
            value_late = [term(blocks[step], mask, value_weight) for mask, blocks in late.items()]
            key_proj = total([key_early[cut]] + key_late).reshape(size, head_local, key_width)
            values = total([value_early[cut]] + value_late).astype(jnp.bfloat16)
            values = values.reshape(size, head_local, value_width)
            at = slice(start, start + size)
            start += size
            first = key_proj[..., :half_width]
            second = key_proj[..., half_width:]
            cos = cosine[at, None, :]
            sin = sine[at, None, :]
            turned = jnp.concatenate([first * cos - second * sin, first * sin + second * cos], -1)
            keys = turned.astype(jnp.bfloat16).astype(jnp.float32)
            weighted = (keys * weighting[at, :, None]).astype(jnp.bfloat16)
            part = jnp.einsum("thd,the->hde", weighted, values, preferred_element_type=jnp.float32)
            state = part if state is None else state + part

    queries = query_new.astype(jnp.float32).reshape(SEQS, head_local, key_width)
    own_query = lax.dynamic_index_in_dim(queries, sp_place // seq_span, 0, keepdims=False)
    own_read = jnp.sum(own_query[:, :, None] * state, axis=1)

    row_count = key_width // sp_size
    blocks = state.astype(jnp.bfloat16).reshape(head_local, sp_size, row_count, value_width)
    blocks = blocks.transpose(1, 0, 2, 3).reshape(sp_size, head_local * row_count, value_width)
    coarse = lax.reduce_precision(own_read, 8, 7)
    reads = jnp.concatenate([coarse, own_read - coarse]).astype(jnp.bfloat16)
    reads = jnp.broadcast_to(reads[None], (sp_size,) + reads.shape)
    got = lax.all_to_all(jnp.concatenate([blocks, reads], axis=1), "sp", 0, 0)
    got = got.astype(jnp.float32).reshape(SEQS, seq_span, -1, value_width).sum(axis=1)
    state_rows = head_local * row_count
    final = got[:, :state_rows].reshape(SEQS, head_local, row_count, value_width)
    state_cache = final.astype(jnp.bfloat16)
    carried = got[:, state_rows : state_rows + head_local] + got[:, state_rows + head_local :]

    keys_next = key_new.astype(jnp.float32).reshape(SEQS, head_local, key_width)
    values_next = value_new.astype(jnp.float32).reshape(SEQS, head_local, value_width)
    own_term = jnp.sum(queries * keys_next, axis=2)[:, :, None] * values_next
    mixed = jnp.exp(decay_exponent)[None, :, None] * carried + own_term
    normed = mixed * lax.rsqrt(jnp.mean(mixed * mixed, axis=2, keepdims=True) + 1e-06)
    normed = normed * norm_gain.reshape(head_local, value_width)[None, :, :]
    return (state_cache, normed.reshape(SEQS, head_local * value_width).astype(jnp.bfloat16))


def solution(mesh):
    in_specs = (
        P("sp", "tp"),
        P(None, "tp"),
        P(None, "tp"),
        P("tp"),
        P(None, "tp"),
        P(None, "tp"),
        P(None, "tp"),
        P("tp"),
    )
    out_specs = (P(None, "tp", "sp", None), P(None, "tp"))
    return jax.shard_map(
        on_device, mesh=mesh, in_specs=in_specs, out_specs=out_specs, check_vma=False
    )
```

```python
import jax
import jax.numpy as jnp
from jax import lax
from jax.sharding import PartitionSpec as P


SEQS = 2
LATE = 2


def turn_tables(position, half_width, scale):
    inverse = 1.0 / 10000.0 ** jnp.linspace(0.0, 1.0, half_width, dtype=jnp.float32)
    angle = position[:, None] * inverse[None, :]
    return jnp.cos(angle) * scale, jnp.sin(angle) * scale


def swap(block, axis, mask):
    size = lax.axis_size(axis)
    return lax.ppermute(block, axis, [(i, i ^ mask) for i in range(size)])


def spread(own, axis):
    size = lax.axis_size(axis)
    bits = [1 << b for b in range(size.bit_length() - 1)]
    rows = own.shape[0] // 2
    halves = []
    for half, order in enumerate((bits, bits[::-1])):
        pieces = {0: [own[half * rows : (half + 1) * rows]]}
        for bit in order:
            for mask in list(pieces):
                blocks = pieces[mask]
                if mask and bit == order[-1]:
                    blocks = [cut for block in blocks for cut in jnp.split(block, LATE)]
                pieces[mask | bit] = []
                for block in blocks:
                    pieces[mask | bit].append(swap(block, axis, bit))
        halves.append(pieces)
    return halves


def on_device(
    layer_input, key_weight, value_weight, decay_exponent, query_new, key_new, value_new, norm_gain
):
    tok_count, feature_local = layer_input.shape
    head_local = decay_exponent.shape[0]
    key_width = key_weight.shape[1] // head_local
    value_width = value_weight.shape[1] // head_local
    half_width = key_width // 2
    sp_size = lax.axis_size("sp")
    seq_span = sp_size // SEQS
    seq_length = tok_count * seq_span
    sp_place = lax.axis_index("sp")
    tp_place = lax.axis_index("tp")

    position = (sp_place % seq_span * tok_count + jnp.arange(tok_count, dtype=jnp.int32)).astype(
        jnp.float32
    )
    cosine, sine = turn_tables(position, half_width, key_width ** (-0.5))
    distance = seq_length - 1.0 - position
    weighting = jnp.exp(decay_exponent[None, :] * distance[:, None])

    def term(piece, mask, weight):
        rows = lax.dynamic_slice_in_dim(weight, (tp_place ^ mask) * feature_local, feature_local)
        return jnp.dot(piece, rows, preferred_element_type=jnp.float32)

    def total(terms):
        result = terms[0]
        for other in terms[1:]:
            result = result + other
        return result

    state = None
    start = 0
    for pieces in spread(layer_input, "tp"):
        early = {mask: blocks[0] for mask, blocks in pieces.items() if len(blocks) == 1}
        late = {mask: blocks for mask, blocks in pieces.items() if len(blocks) > 1}
        key_early = total([term(piece, mask, key_weight) for mask, piece in early.items()])
        value_early = total([term(piece, mask, value_weight) for mask, piece in early.items()])
        size = key_early.shape[0] // LATE
        for step in range(LATE):
            cut = slice(step * size, (step + 1) * size)
            key_late = [term(blocks[step], mask, key_weight) for mask, blocks in late.items()]
            value_late = [term(blocks[step], mask, value_weight) for mask, blocks in late.items()]
            key_proj = total([key_early[cut]] + key_late).reshape(size, head_local, key_width)
            values = total([value_early[cut]] + value_late).astype(jnp.bfloat16)
            values = values.reshape(size, head_local, value_width)
            at = slice(start, start + size)
            start += size
            first = key_proj[..., :half_width]
            second = key_proj[..., half_width:]
            cos = cosine[at, None, :]
            sin = sine[at, None, :]
            turned = jnp.concatenate([first * cos - second * sin, first * sin + second * cos], -1)
            keys = turned.astype(jnp.bfloat16).astype(jnp.float32)
            weighted = (keys * weighting[at, :, None]).astype(jnp.bfloat16)
            part = jnp.einsum("thd,the->hde", weighted, values, preferred_element_type=jnp.float32)
            state = part if state is None else state + part

    queries = query_new.astype(jnp.float32).reshape(SEQS, head_local, key_width)
    own_query = lax.dynamic_index_in_dim(queries, sp_place // seq_span, 0, keepdims=False)
    own_read = jnp.sum(own_query[:, :, None] * state, axis=1)

    row_count = key_width // sp_size
    blocks = state.astype(jnp.bfloat16).reshape(head_local, sp_size, row_count, value_width)
    blocks = blocks.transpose(1, 0, 2, 3).reshape(sp_size, head_local * row_count, value_width)
    coarse = lax.reduce_precision(own_read, 8, 7)
    reads = jnp.concatenate([coarse, own_read - coarse]).astype(jnp.bfloat16)
    place = [sp_place ^ mask for mask in range(sp_size)]
    mine = [
        jnp.concatenate([lax.dynamic_index_in_dim(blocks, to, 0, keepdims=False), reads])
        for to in place
    ]
    got = [mine[0]] + [swap(mine[mask], "sp", mask) for mask in range(1, sp_size)]
    member = sp_place // seq_span
    near = sum(block.astype(jnp.float32) for block in got[:seq_span])
    far = sum(block.astype(jnp.float32) for block in got[seq_span:])
    got = jnp.stack([jnp.where(member == 0, near, far), jnp.where(member == 0, far, near)])
    state_rows = head_local * row_count
    final = got[:, :state_rows].reshape(SEQS, head_local, row_count, value_width)
    state_cache = final.astype(jnp.bfloat16)
    carried = got[:, state_rows : state_rows + head_local] + got[:, state_rows + head_local :]

    keys_next = key_new.astype(jnp.float32).reshape(SEQS, head_local, key_width)
    values_next = value_new.astype(jnp.float32).reshape(SEQS, head_local, value_width)
    own_term = jnp.sum(queries * keys_next, axis=2)[:, :, None] * values_next
    mixed = jnp.exp(decay_exponent)[None, :, None] * carried + own_term
    normed = mixed * lax.rsqrt(jnp.mean(mixed * mixed, axis=2, keepdims=True) + 1e-06)
    normed = normed * norm_gain.reshape(head_local, value_width)[None, :, :]
    return (state_cache, normed.reshape(SEQS, head_local * value_width).astype(jnp.bfloat16))


def solution(mesh):
    in_specs = (
        P("sp", "tp"),
        P(None, "tp"),
        P(None, "tp"),
        P("tp"),
        P(None, "tp"),
        P(None, "tp"),
        P(None, "tp"),
        P("tp"),
    )
    out_specs = (P(None, "tp", "sp", None), P(None, "tp"))
    return jax.shard_map(
        on_device, mesh=mesh, in_specs=in_specs, out_specs=out_specs, check_vma=False
    )
```
